32 devices in a mesh: sp: 8 (over z, y), tp: 4 (over x, core).
Axes of the slice: x: 2, y: 2, z: 4, core: 2. Of those that a mesh axis runs over, the one named last changes fastest.
Arguments:
- resid: bfloat16 [6144, 2048], P(('sp', 'tp')), may hold values from -6 to 6
- query: bfloat16 [6144, 1024], P('sp', 'tp'), may hold values from -6 to 6
- keys: bfloat16 [6144, 1024], P('sp', 'tp'), may hold values from -6 to 6
- values: bfloat16 [6144, 1024], P('sp', 'tp'), may hold values from -6 to 6
- out_gate: bfloat16 [6144, 1024], P(('sp', 'tp')), may hold values from -6 to 6
- forget_pre: float32 [4, 6144], P('tp', 'sp'), may hold values from 0 to 16
- input_pre: float32 [4, 6144], P('tp', 'sp'), may hold values from -4 to 130
- head_gain: float32 [1024], replicated, may hold values from 0.1 to 1.9
- out_proj: bfloat16 [1024, 2048], replicated, may hold values from -0.1875 to 0.1875
- ffn_gain: float32 [2048], replicated, may hold values from 0.1 to 1.9
- routes: int32 [6144, 2], P(('sp', 'tp')), may hold values from 0 to 7, all different within a row; in each aligned block of 96 rows (0 to 95, 96 to 191, ...) at most 48 rows name the same one
- route_scores: float32 [6144, 2], P(('sp', 'tp')), may hold values from 0.1 to 1
- w_gate: bfloat16 [8, 2048, 512], P('sp'), may hold values from -0.125 to 0.125
- w_up: bfloat16 [8, 2048, 512], P('sp'), may hold values from -0.125 to 0.125
- w_down: bfloat16 [8, 512, 2048], P('sp'), may hold values from -0.25 to 0.25
Outputs:
- layer_out: bfloat16 [6144, 2048], P(('sp', 'tp'))
The draws below stay inside these ranges and needn't reach their ends.
Inputs may be any that keep to these rules, and one draw needn't show every extreme that they name: `routes`: each row names 2 different experts; in each aligned block of 96 rows no expert is named by more than 48 rows, a bound that some block reaches.
All inputs are finite; a program needn't handle non-finite values.
Results may differ from the reference program's by a relative error of at most 0.0095.
Values may be sent and summed in bfloat16 or wider, within the bound.
A program may use at most 128 MiB of HBM per device.

```python
import math
import jax
import jax.numpy as jnp
import numpy as np
from jax import lax

D = 2048
CELL_HEADS = 4
HEAD_DIM = 256
MDIM = 1024
FF = 512
EXPERTS = 8
TOPK = 2
BLOCK = 64
TOK_DEV = 768
SEQUENCE_TOKENS = 6144
HALF = 96
CAP = 48


def draw_forget_pre(key, part):
    split_random_keys = jax.random.split(jax.random.fold_in(key, 17), 5)
    head_order = jax.random.permutation(split_random_keys[0], CELL_HEADS)
    fast_heads = head_order < CELL_HEADS // 2
    jitter = jnp.clip(jax.random.normal(split_random_keys[1], (CELL_HEADS, SEQUENCE_TOKENS), jnp.float32) * 0.7, -2.4, 2.4)
    base_level = jnp.where(fast_heads, jnp.log(100.0), jnp.log(1.0 * SEQUENCE_TOKENS) + 1.5).astype(jnp.float32)
    factor = jax.random.uniform(split_random_keys[2], (SEQUENCE_TOKENS // TOK_DEV,), jnp.float32, 0.0, jnp.log(4.0))
    slow_part = jnp.repeat(factor, TOK_DEV, total_repeat_length=SEQUENCE_TOKENS)
    output_values = base_level[:, None] - slow_part[None, :] + jitter
    outlier_position = jax.random.randint(split_random_keys[3], (3,), 0, SEQUENCE_TOKENS)
    outlier_mask = jnp.any(jnp.arange(SEQUENCE_TOKENS)[:, None] == outlier_position[None, :], axis=1)
    outlier_value = jax.random.uniform(split_random_keys[4], (CELL_HEADS, SEQUENCE_TOKENS), jnp.float32, 0.0, 1.39)
    return jnp.where(outlier_mask[None, :], outlier_value, output_values)


def draw_input_pre(key, part):
    split_random_keys = jax.random.split(jax.random.fold_in(key, 29), 1)
    return jnp.clip(jax.random.normal(split_random_keys[0], (CELL_HEADS, SEQUENCE_TOKENS), jnp.float32), -4.0, 4.0)


def block_levels(stream_key, dims, pieces, least, largest):
    factor_of = 1.0
    for position, parts in pieces:
        steps = jax.random.uniform(jax.random.fold_in(jax.random.fold_in(stream_key, 6), position), (parts,), jnp.float32, least / len(pieces), largest / len(pieces))
        factor_of = factor_of * jnp.repeat(jnp.exp(steps), dims[position] // parts).reshape((-1,) + (1,) * (len(dims) - 1 - position))
    return factor_of


def shared_out(rng, own, number, rows, count, top, reach, skew):
    sequence = jax.random.permutation(rng, count)
    packed, ordinary = shares(count, rows * top, reach, skew, True), shares(count, rows * top, reach, skew, False)
    places = jnp.arange(count)

    def named(sizes, rotation):
        used = int((sizes > 0).sum())
        fixed = max(1, used // 4)
        moved = fixed + (places - fixed + rotation * (used - fixed)) % max(1, count - fixed)
        return jnp.zeros((count,), jnp.int32).at[sequence[jnp.where(places < fixed, places, moved)]].set(jnp.asarray(sizes, jnp.int32))

    sizes = jnp.where(number % 4 == 0, named(packed, number // 4), named(ordinary, number - number // 4 - 1))
    mixed = jax.random.permutation(jax.random.fold_in(own, 3), count)
    donor, sink = mixed[0:count // 2 * 2:2], mixed[1:count // 2 * 2:2]
    margin = jnp.minimum(sizes[donor] - 1, reach - sizes[sink]) // 2
    margin = jnp.where((donor == sequence[0]) | (sink == sequence[0]) | (sizes[sink] == 0), 0, jnp.maximum(margin, 0))
    moved = jax.random.randint(jax.random.fold_in(own, 4), (count // 2,), 0, 1 << 20) % (margin + 1)
    sizes = sizes.at[donor].add(-moved).at[sink].add(moved)
    labels = jnp.searchsorted(jnp.cumsum(sizes), jnp.arange(rows * top), side="right").astype(jnp.int32)
    grid = labels.reshape(top, rows).T
    grid = grid[jax.random.permutation(jax.random.fold_in(own, 1), rows)]
    rotation = jax.random.randint(jax.random.fold_in(own, 2), (rows, 1), 0, top)
    return jnp.take_along_axis(grid, (jnp.arange(top)[None, :] + rotation) % top, axis=1)


def shares(count, total, limit, skew, full):
    loads = [(1 << 20) // math.isqrt(rank ** skew) + 1 for rank in range(1, count + 1)]
    largest = limit if full else min(limit, max(-(-total // count), total * loads[0] // sum(loads)))
    least = 1 if total - largest >= count - 1 else 0
    counts, spare = [largest] + [least] * (count - 1), total - largest - least * (count - 1)
    while spare > 0:
        movable = [i for i in range(1, count) if counts[i] < largest] or [i for i in range(1, count) if counts[i] < limit]
        pool, left = sum([loads[i] for i in movable]), spare
        for i in movable:
            addition = min(limit - counts[i], max(1, left * loads[i] // pool), spare)
            counts[i] = counts[i] + addition
            spare = spare - addition
    return np.array(counts)


def centred(key, extent, spread, limit, shards=(), held_as=jnp.bfloat16):
    values = spread * jax.random.normal(key, extent, jnp.float32)
    if shards:
        values = values * block_levels(key, extent, shards, -0.22, 0.18)
    return jnp.clip(values, -limit, limit).astype(held_as)


def setup_inputs(seed: int = 0) -> dict:
    key_list = jax.random.split(jax.random.key(seed), 16)
    resid = centred(key_list[0], (SEQUENCE_TOKENS, D), 1.0, 6.0, ((0, 32),))
    query = centred(key_list[1], (SEQUENCE_TOKENS, MDIM), 1.0, 6.0, ((0, 8), (1, 4)))
    keys = centred(key_list[2], (SEQUENCE_TOKENS, MDIM), 1.0, 6.0, ((0, 8), (1, 4)))
    values = centred(key_list[3], (SEQUENCE_TOKENS, MDIM), 1.0, 6.0, ((0, 8), (1, 4)))
    out_gate = centred(key_list[4], (SEQUENCE_TOKENS, MDIM), 1.0, 6.0, ((0, 32),))
    forget_pre = draw_forget_pre(jax.random.fold_in(key_list[15], 71), 0)
    input_pre = draw_input_pre(jax.random.fold_in(key_list[15], 71), 0)
    head_gain = jnp.clip(1.0 + 0.18 * jax.random.normal(key_list[7], (MDIM,), jnp.float32), 0.1, 1.9)
    out_proj = centred(key_list[8], (MDIM, D), MDIM ** -0.5, 0.1875)
    ffn_gain = jnp.clip(1.0 + 0.18 * jax.random.normal(key_list[9], (D,), jnp.float32), 0.1, 1.9)
    routes_keys = jax.random.split(jax.random.fold_in(key_list[10], 1), SEQUENCE_TOKENS // HALF)
    routes_turns = jax.random.permutation(jax.random.fold_in(key_list[10], 3), SEQUENCE_TOKENS // HALF)
    routes = jax.vmap(lambda own, number: shared_out(jax.random.fold_in(key_list[10], 2), own, number, HALF, EXPERTS, TOPK, CAP, 1))(routes_keys, routes_turns).reshape((SEQUENCE_TOKENS, TOPK))
    route_scores = jnp.clip(0.1 + 0.9 * jax.random.uniform(key_list[11], (SEQUENCE_TOKENS, TOPK), jnp.float32) ** block_levels(key_list[11], (SEQUENCE_TOKENS, TOPK), ((0, 32),), -0.2, 0.2), 0.1, 1.0)
    w_gate = centred(key_list[12], (EXPERTS, D, FF), D ** -0.5, 0.125, ((0, 8),))
    w_up = centred(key_list[13], (EXPERTS, D, FF), D ** -0.5, 0.125, ((0, 8),))
    w_down = centred(key_list[14], (EXPERTS, FF, D), FF ** -0.5, 0.25, ((0, 8),))
    return {"resid": resid, "query": query, "keys": keys, "values": values, "out_gate": out_gate, "forget_pre": forget_pre, "input_pre": input_pre, "head_gain": head_gain, "out_proj": out_proj, "ffn_gain": ffn_gain, "routes": routes, "route_scores": route_scores, "w_gate": w_gate, "w_up": w_up, "w_down": w_down}


EPS = 1e-06
HIGHEST = lax.Precision.HIGHEST

def block_pass(query, keys, values, log_forget, log_input, state):
    seq_len, head_width = query.shape
    blocks = seq_len // BLOCK
    key_scale = head_width ** (-0.5)
    causal = jnp.tril(jnp.ones((BLOCK, BLOCK), dtype=bool))

    def block_step(state_in, inputs):
        state_mat, state_vec, max_log = state_in
        q_block, k_block, v_block, forget_blk, input_blk = inputs
        cum_log = jnp.cumsum(forget_blk)
        block_total = cum_log[-1]
        log_mat = jnp.where(causal, cum_log[:, None] - cum_log[None, :] + input_blk[None, :], -jnp.inf)
        inter_log = cum_log + max_log
        row_max = jnp.maximum(inter_log, lax.optimization_barrier(jnp.max(log_mat, axis=1)))
        weight_mat = jnp.exp(log_mat - row_max[:, None])
        carry_weight = jnp.exp(inter_log - row_max)
        scores = jnp.dot(q_block, k_block.T, preferred_element_type=jnp.float32) * key_scale
        weights_blk = (scores * weight_mat).astype(jnp.bfloat16)
        q_float = q_block.astype(jnp.float32)
        numerator = carry_weight[:, None] * jnp.dot(q_float, state_mat, precision=HIGHEST) + jnp.dot(weights_blk, v_block, preferred_element_type=jnp.float32)
        denominator = carry_weight * jnp.dot(q_float, state_vec, precision=HIGHEST) + lax.optimization_barrier(jnp.sum(weights_blk.astype(jnp.float32), axis=1))
        log_keep = block_total - cum_log + input_blk
        new_max = jnp.maximum(block_total + max_log, jnp.max(log_keep))
        keep_weight = jnp.exp(log_keep - new_max)
        decay_now = jnp.exp(block_total + max_log - new_max)
        k_float = k_block.astype(jnp.float32) * key_scale
        state_mat = decay_now * state_mat + jnp.dot((k_float * keep_weight[:, None]).T, v_block.astype(jnp.float32), precision=HIGHEST)
        state_vec = decay_now * state_vec + jnp.dot(keep_weight, k_float, precision=HIGHEST)
        return ((state_mat, state_vec, new_max), (numerator, denominator, row_max))

    def to_blocks(array_in):
        return array_in.reshape((blocks, BLOCK) + array_in.shape[1:])
    ignored, outputs = lax.scan(block_step, state, (to_blocks(query), to_blocks(keys), to_blocks(values), to_blocks(log_forget), to_blocks(log_input)))
    numerator, denominator, row_max = outputs
    return (numerator.reshape(seq_len, head_width), denominator.reshape(seq_len), row_max.reshape(seq_len))

def reference(resid, query, keys, values, out_gate, forget_pre, input_pre, head_gain, out_proj, ffn_gain, routes, route_scores, w_gate, w_up, w_down):
    log_forget = jax.nn.log_sigmoid(forget_pre)
    start_state = (jnp.zeros((HEAD_DIM, HEAD_DIM), jnp.float32), jnp.zeros((HEAD_DIM,), jnp.float32), jnp.zeros((), jnp.float32))
    head_outs = []
    for head_idx in range(CELL_HEADS):
        col_start = head_idx * HEAD_DIM
        col_end = col_start + HEAD_DIM
        numerator, denominator, row_max = block_pass(query[:, col_start:col_end], keys[:, col_start:col_end], values[:, col_start:col_end], log_forget[head_idx], input_pre[head_idx], start_state)
        hidden = numerator / jnp.maximum(jnp.abs(denominator), jnp.exp(-row_max))[:, None]
        head_outs.append(hidden)
    cell_rows = lax.optimization_barrier(jnp.concatenate(head_outs, axis=1).astype(jnp.bfloat16))
    cell_float = cell_rows.astype(jnp.float32)
    headed = cell_float * lax.rsqrt(lax.optimization_barrier(jnp.mean(cell_float * cell_float, axis=1, keepdims=True)) + EPS) * head_gain[None, :]
    gated_out = (headed * jax.nn.sigmoid(out_gate.astype(jnp.float32))).astype(jnp.bfloat16)
    after_mix = resid.astype(jnp.float32) + jnp.dot(gated_out, out_proj, preferred_element_type=jnp.float32)
    normed_rows = (after_mix * lax.rsqrt(lax.optimization_barrier(jnp.mean(after_mix * after_mix, axis=1, keepdims=True)) + EPS) * ffn_gain[None, :]).astype(jnp.bfloat16)
    flat_ids = routes.reshape(-1).astype(jnp.int32)
    one_hot = (flat_ids[:, None] == jnp.arange(EXPERTS, dtype=jnp.int32)[None, :]).astype(jnp.int32)
    slot_rank = lax.optimization_barrier(jnp.sum((jnp.cumsum(one_hot, axis=0) - 1) * one_hot, axis=1)).astype(jnp.int32)
    most_rows = SEQUENCE_TOKENS // HALF * CAP
    index_table = jnp.zeros((EXPERTS, most_rows), jnp.int32).at[flat_ids, slot_rank].set(jnp.arange(flat_ids.shape[0], dtype=jnp.int32) // TOPK)

    def one_expert(operands):
        row_picks, gate_mat, up_mat, down_mat = operands
        tok_rows = normed_rows[row_picks]
        gate_pre = jnp.dot(tok_rows, gate_mat, preferred_element_type=jnp.float32)
        up_pre = jnp.dot(tok_rows, up_mat, preferred_element_type=jnp.float32)
        active = (jax.nn.silu(gate_pre) * up_pre).astype(jnp.bfloat16)
        return jnp.dot(active, down_mat, preferred_element_type=jnp.float32).astype(jnp.bfloat16)
    expert_out = lax.map(one_expert, (index_table, w_gate, w_up, w_down))
    assigned = expert_out[flat_ids, slot_rank].astype(jnp.float32).reshape(SEQUENCE_TOKENS, TOPK, D)
    route_weight = route_scores / lax.optimization_barrier(jnp.sum(route_scores, axis=1, keepdims=True))
    combined = lax.optimization_barrier(jnp.sum(assigned * route_weight[:, :, None], axis=1))
    return (after_mix + combined).astype(jnp.bfloat16)
```

```python
import functools

import jax
import jax.numpy as jnp
from jax import lax
from jax.experimental import pallas as pl
from jax.experimental.pallas import tpu as pltpu
from jax.sharding import PartitionSpec as P

BLOCK = 64


EPS = 1e-06
FLOOR_LOG = -1e30
HIGHEST = lax.Precision.HIGHEST


EXTRA = 8
VMEM_LIMIT = 56 * 1024 * 1024


def col_mask(first_row, rows, cols):
    row = lax.broadcasted_iota(jnp.int32, (rows, cols), 0) + first_row
    col = lax.broadcasted_iota(jnp.int32, (rows, cols), 1)
    return row, col


def split_two(a):
    high = a.astype(jnp.bfloat16)
    return high, (a - high.astype(jnp.float32)).astype(jnp.bfloat16)


def log_rows(forget_ref, input_ref):
    pre = forget_ref[...]
    log_forget = jnp.minimum(pre, 0.0) - jnp.log1p(jnp.exp(-jnp.abs(pre)))
    seq_len = pre.shape[1]
    row, col = col_mask(0, seq_len, seq_len)
    upper = jnp.where(row <= col, 1.0, 0.0).astype(jnp.bfloat16)
    one, rest = split_two(log_forget)
    two, three = split_two(log_forget - one.astype(jnp.float32))
    stacked = jnp.concatenate([one, two, three, jnp.zeros((13, seq_len), jnp.bfloat16)], axis=0)
    sums = jnp.dot(stacked, upper, preferred_element_type=jnp.float32)
    cum_row = sums[0:1] + sums[1:2] + sums[2:3]
    return log_forget, cum_row, input_ref[...] - cum_row


def cell_state_kernel(k_ref, v_ref, forget_ref, input_ref, state_ref):
    width = k_ref.shape[1]
    seq_len = k_ref.shape[0]
    log_forget, cum_row, gap_row = log_rows(forget_ref, input_ref)
    total = jnp.sum(log_forget, axis=1, keepdims=True)
    top = jnp.max(gap_row, axis=1, keepdims=True)
    keep_row = jnp.exp(gap_row - top) * width ** (-0.5)
    k_turned = k_ref[...].astype(jnp.float32).T
    weighted = k_turned * keep_row
    high, low = split_two(weighted)
    v = v_ref[...]
    state_ref[0:width, :] = jnp.dot(high, v, preferred_element_type=jnp.float32) + jnp.dot(
        low, v, preferred_element_type=jnp.float32
    )
    vector = jnp.dot(
        jnp.broadcast_to(keep_row, (8, seq_len)),
        k_ref[...].astype(jnp.float32),
        precision=HIGHEST,
        preferred_element_type=jnp.float32,
    )[0:1]
    lanes = jnp.zeros((1, width), jnp.float32)
    state_ref[width : width + EXTRA, :] = jnp.concatenate(
        [vector, lanes + total, lanes + total + top, jnp.zeros((EXTRA - 3, width), jnp.float32)],
        axis=0,
    )


def cell_local_kernel(q_ref, k_ref, v_ref, forget_ref, input_ref, num_ref, aux_ref, *, tile):
    seq_len, width = q_ref.shape
    log_forget, cum_row, gap_row = log_rows(forget_ref, input_ref)
    for first in range(0, seq_len, tile):
        span = first + tile
        row, col = col_mask(first, tile, span)
        causal = col <= row
        own = (col // BLOCK) == (row // BLOCK)
        gap = jnp.where(causal, gap_row[:, :span], -jnp.inf)
        top = jnp.max(gap, axis=1, keepdims=True)
        cum = jnp.sum(jnp.where(causal, log_forget[:, :span], 0.0), axis=1, keepdims=True)
        scores = lax.dot_general(
            q_ref[first:span, :],
            k_ref[0:span, :],
            (((1,), (1,)), ((), ())),
            preferred_element_type=jnp.float32,
        ) * width ** (-0.5)
        weights = scores * jnp.exp(gap - top)
        high = weights.astype(jnp.bfloat16)
        high_float = high.astype(jnp.float32)
        low_float = jnp.where(own, 0.0, weights - high_float)
        v = v_ref[0:span, :]
        num_ref[first:span, :] = jnp.dot(high, v, preferred_element_type=jnp.float32) + jnp.dot(
            low_float.astype(jnp.bfloat16), v, preferred_element_type=jnp.float32
        )
        den = jnp.sum(high_float + low_float, axis=1, keepdims=True)
        lane = lax.broadcasted_iota(jnp.int32, (tile, 128), 1)
        aux_ref[first:span, :] = jnp.where(lane == 0, den, jnp.where(lane == 1, top, cum))


def cell_join_kernel(q_ref, num_ref, aux_ref, states_ref, rows_ref, mat_ref, *, axis):
    width = q_ref.shape[1]
    place = lax.axis_index(axis)
    mat_ref[...] = jnp.zeros_like(mat_ref)

    def join(step, carry):
        vector, old_max = carry
        extra = states_ref[step, width : width + EXTRA, :]
        new_max, total = extra[2:3], extra[1:2]
        joined = jnp.maximum(total + old_max, new_max)
        keep_old = jnp.exp(total + old_max - joined)
        keep_new = jnp.exp(new_max - joined)
        mat_ref[...] = keep_old * mat_ref[...] + keep_new * states_ref[step, 0:width, :]
        return keep_old * vector + keep_new * extra[0:1], joined

    vector, far_max = lax.fori_loop(
        0,
        place,
        join,
        (jnp.zeros((1, width), jnp.float32), jnp.full((1, width), FLOOR_LOG, jnp.float32)),
    )
    aux = aux_ref[...]
    den, top, cum = aux[:, 0:1], aux[:, 1:2], aux[:, 2:3]
    far = far_max[:, 0:1]
    joined = jnp.maximum(top, far)
    keep_own = jnp.exp(top - joined)
    keep_far = jnp.exp(far - joined)
    q_float = q_ref[...].astype(jnp.float32)
    one, rest = split_two(mat_ref[...])
    two, three = split_two(mat_ref[...] - one.astype(jnp.float32))
    q = q_ref[...]
    far_num = (
        jnp.dot(q, one, preferred_element_type=jnp.float32)
        + jnp.dot(q, two, preferred_element_type=jnp.float32)
        + jnp.dot(q, three, preferred_element_type=jnp.float32)
    )
    far_den = jnp.sum(q_float * vector, axis=1, keepdims=True)
    numerator = keep_own * num_ref[...] + keep_far * far_num
    denominator = keep_own * den + keep_far * far_den
    divisor = jnp.maximum(jnp.abs(denominator), jnp.exp(-(cum + joined)))
    rows_ref[...] = (numerator / divisor).astype(rows_ref.dtype)


def run_cell(query, keys, values, forget_pre, input_pre, riders):
    seq_len, width = query.shape
    params = pltpu.CompilerParams(vmem_limit_bytes=VMEM_LIMIT)
    state = pl.pallas_call(
        cell_state_kernel,
        out_shape=jax.ShapeDtypeStruct((width + EXTRA, width), jnp.float32),
        compiler_params=params,
        cost_estimate=pl.CostEstimate(flops=10**9, bytes_accessed=2**20, transcendentals=0),
        name="cell_state",
    )(keys, values, forget_pre, input_pre)
    if riders is not None:
        state = jnp.concatenate([state, riders], axis=0)
    gathered = lax.all_gather(state, "sp")
    tile = 4 * BLOCK if seq_len % (4 * BLOCK) == 0 else BLOCK
    numerator, aux = pl.pallas_call(
        functools.partial(cell_local_kernel, tile=tile),
        out_shape=(
            jax.ShapeDtypeStruct((seq_len, width), jnp.float32),
            jax.ShapeDtypeStruct((seq_len, 128), jnp.float32),
        ),
        compiler_params=params,
        cost_estimate=pl.CostEstimate(flops=5 * 10**9, bytes_accessed=2**21, transcendentals=0),
        name="cell_local",
    )(query, keys, values, forget_pre, input_pre)
    rows = pl.pallas_call(
        functools.partial(cell_join_kernel, axis="sp"),
        out_shape=jax.ShapeDtypeStruct((seq_len, width), jnp.bfloat16),
        scratch_shapes=[pltpu.VMEM((width, width), jnp.float32)],
        compiler_params=params,
        name="cell_join",
    )(query, numerator, aux, gathered[:, : width + EXTRA])
    return rows, gathered[:, width + EXTRA :]


def slot_select(expert_ids, expert_count, capacity):
    flat_ids = expert_ids.reshape(-1)
    one_hot = (flat_ids[:, None] == jnp.arange(expert_count, dtype=jnp.int32)[None, :]).astype(
        jnp.int32
    )
    slot_rank = jnp.sum((jnp.cumsum(one_hot, axis=0) - 1) * one_hot, axis=1)
    target = flat_ids * capacity + slot_rank
    return (
        jnp.arange(expert_count * capacity, dtype=jnp.int32)[:, None] == target[None, :]
    ).astype(jnp.bfloat16)


def run_experts(arrived, w_gate, w_up, w_down, sources):
    local_count = w_gate.shape[0]
    grouped = arrived.reshape(sources, local_count, arrived.shape[1], arrived.shape[2])
    gate_pre = jnp.einsum("pesd,edf->pesf", grouped, w_gate, preferred_element_type=jnp.float32)
    up_pre = jnp.einsum("pesd,edf->pesf", grouped, w_up, preferred_element_type=jnp.float32)
    active = (jax.nn.silu(gate_pre) * up_pre).astype(jnp.bfloat16)
    result = jnp.einsum(
        "pesf,efd->pesd", active, w_down, preferred_element_type=jnp.float32
    ).astype(jnp.bfloat16)
    return result.reshape(arrived.shape)


def shards(
    resid,
    query,
    keys,
    values,
    out_gate,
    forget_pre,
    input_pre,
    head_gain,
    out_proj,
    ffn_gain,
    routes,
    route_scores,
    w_gate,
    w_up,
    w_down,
):
    head_width = query.shape[1]
    row_count, route_count = routes.shape
    sources = lax.axis_size("sp")
    local_experts = w_gate.shape[0]
    expert_count = local_experts * sources
    half_rows = row_count // 2
    capacity = max(2, 2 * half_rows * route_count // expert_count)
    whole_rows = local_experts == 1 and row_count <= 2 * expert_count * capacity
    whole_rows = whole_rows and sources * row_count <= 8 * row_count and row_count <= head_width
    route_weight = route_scores / jnp.sum(route_scores, axis=1, keepdims=True)
    riders = None
    if whole_rows:
        named = routes[:, :, None] == jnp.arange(expert_count, dtype=routes.dtype)[None, None, :]
        per_expert = jnp.sum(jnp.where(named, route_weight[:, :, None], 0.0), axis=1).T
        riders = jnp.pad(
            per_expert, ((0, -expert_count % 8), (0, head_width - row_count))
        )
    cell_rows, ridden = run_cell(query, keys, values, forget_pre, input_pre, riders)
    token_rows = lax.all_to_all(cell_rows, "tp", split_axis=0, concat_axis=1, tiled=True)
    cell_float = token_rows.astype(jnp.float32)
    headed = (
        cell_float
        * lax.rsqrt(jnp.mean(cell_float * cell_float, axis=1, keepdims=True) + EPS)
        * head_gain[None, :]
    )
    gated_out = (headed * jax.nn.sigmoid(out_gate.astype(jnp.float32))).astype(jnp.bfloat16)
    after_mix = resid.astype(jnp.float32) + jnp.dot(
        gated_out, out_proj, preferred_element_type=jnp.float32
    )
    normed_rows = (
        after_mix
        * lax.rsqrt(jnp.mean(after_mix * after_mix, axis=1, keepdims=True) + EPS)
        * ffn_gain[None, :]
    ).astype(jnp.bfloat16)
    if whole_rows:
        here = lax.axis_index("sp")
        weights = lax.dynamic_index_in_dim(ridden, here, 1, False)[:, :row_count]
        weights = weights.reshape(sources * row_count, 1)
        arrived = lax.all_gather(normed_rows, "sp", axis=0, tiled=True)
        gate_pre = jnp.dot(arrived, w_gate[0], preferred_element_type=jnp.float32)
        up_pre = jnp.dot(arrived, w_up[0], preferred_element_type=jnp.float32)
        active = (jax.nn.silu(gate_pre) * up_pre).astype(jnp.bfloat16)
        result = jnp.dot(active, w_down[0], preferred_element_type=jnp.float32)
        weighted = (result * weights).astype(jnp.bfloat16)
        combined = lax.psum_scatter(weighted, "sp", scatter_dimension=0, tiled=True)
        return (after_mix + combined.astype(jnp.float32)).astype(jnp.bfloat16)
    selects = [
        slot_select(
            routes[half_idx * half_rows : (half_idx + 1) * half_rows], expert_count, capacity
        )
        for half_idx in range(2)
    ]

    def pack_rows(half_idx):
        selection = (
            selects[half_idx].reshape(expert_count * capacity, half_rows, route_count).sum(axis=2)
        )
        packed = jnp.dot(
            selection,
            normed_rows[half_idx * half_rows : (half_idx + 1) * half_rows],
            preferred_element_type=jnp.float32,
        )
        return packed.astype(jnp.bfloat16).reshape(expert_count, capacity, normed_rows.shape[1])

    send_rows = jnp.concatenate([pack_rows(0), pack_rows(1)], axis=1)
    finished = run_experts(
        lax.all_to_all(send_rows, "sp", split_axis=0, concat_axis=0, tiled=True),
        w_gate,
        w_up,
        w_down,
        sources,
    )
    returned = lax.all_to_all(finished, "sp", split_axis=0, concat_axis=0, tiled=True)
    answers = [returned[:, :capacity], returned[:, capacity:]]
    pieces = []
    for half_idx in range(2):
        gathered = lax.dot_general(
            selects[half_idx],
            answers[half_idx].reshape(expert_count * capacity, -1),
            (((0,), (0,)), ((), ())),
            preferred_element_type=jnp.float32,
        )
        weights_half = route_weight[half_idx * half_rows : (half_idx + 1) * half_rows]
        pieces.append(
            jnp.sum(gathered.reshape(half_rows, route_count, -1) * weights_half[:, :, None], axis=1)
        )
    return (after_mix + jnp.concatenate(pieces, axis=0)).astype(jnp.bfloat16)


def solution(mesh):
    placed = (
        P(("sp", "tp"), None),
        P("sp", "tp"),
        P("sp", "tp"),
        P("sp", "tp"),
        P(("sp", "tp"), None),
        P("tp", "sp"),
        P("tp", "sp"),
        P(),
        P(),
        P(),
        P(("sp", "tp"), None),
        P(("sp", "tp"), None),
        P("sp", None, None),
        P("sp", None, None),
        P("sp", None, None),
    )
    return jax.shard_map(
        shards, mesh=mesh, in_specs=placed, out_specs=P(("sp", "tp"), None), check_vma=False
    )
```

```python
import functools

import jax
import jax.numpy as jnp
from jax import lax
from jax.experimental import pallas as pl
from jax.experimental.pallas import tpu as pltpu
from jax.sharding import PartitionSpec as P

BLOCK = 64


EPS = 1e-06
FLOOR_LOG = -1e30
HIGHEST = lax.Precision.HIGHEST


EXTRA = 8
VMEM_LIMIT = 56 * 1024 * 1024


def col_mask(first_row, rows, cols):
    row = lax.broadcasted_iota(jnp.int32, (rows, cols), 0) + first_row
    col = lax.broadcasted_iota(jnp.int32, (rows, cols), 1)
    return row, col


def split_two(a):
    high = a.astype(jnp.bfloat16)
    return high, (a - high.astype(jnp.float32)).astype(jnp.bfloat16)


def log_rows(forget_ref, input_ref):
    pre = forget_ref[...]
    log_forget = jnp.minimum(pre, 0.0) - jnp.log1p(jnp.exp(-jnp.abs(pre)))
    seq_len = pre.shape[1]
    row, col = col_mask(0, seq_len, seq_len)
    upper = jnp.where(row <= col, 1.0, 0.0).astype(jnp.bfloat16)
    one, rest = split_two(log_forget)
    two, three = split_two(log_forget - one.astype(jnp.float32))
    stacked = jnp.concatenate([one, two, three, jnp.zeros((13, seq_len), jnp.bfloat16)], axis=0)
    sums = jnp.dot(stacked, upper, preferred_element_type=jnp.float32)
    cum_row = sums[0:1] + sums[1:2] + sums[2:3]
    return log_forget, cum_row, input_ref[...] - cum_row


def cell_state_kernel(k_ref, v_ref, forget_ref, input_ref, state_ref):
    width = k_ref.shape[1]
    seq_len = k_ref.shape[0]
    log_forget, cum_row, gap_row = log_rows(forget_ref, input_ref)
    total = jnp.sum(log_forget, axis=1, keepdims=True)
    top = jnp.max(gap_row, axis=1, keepdims=True)
    keep_row = jnp.exp(gap_row - top) * width ** (-0.5)
    k_turned = k_ref[...].astype(jnp.float32).T
    weighted = k_turned * keep_row
    high, low = split_two(weighted)
    v = v_ref[...]
    state_ref[0:width, :] = jnp.dot(high, v, preferred_element_type=jnp.float32) + jnp.dot(
        low, v, preferred_element_type=jnp.float32
    )
    vector = jnp.dot(
        jnp.broadcast_to(keep_row, (8, seq_len)),
        k_ref[...].astype(jnp.float32),
        precision=HIGHEST,
        preferred_element_type=jnp.float32,
    )[0:1]
    lanes = jnp.zeros((1, width), jnp.float32)
    state_ref[width : width + EXTRA, :] = jnp.concatenate(
        [vector, lanes + total, lanes + total + top, jnp.zeros((EXTRA - 3, width), jnp.float32)],
        axis=0,
    )


def cell_local_kernel(q_ref, k_ref, v_ref, forget_ref, input_ref, num_ref, aux_ref, *, tile):
    seq_len, width = q_ref.shape
    log_forget, cum_row, gap_row = log_rows(forget_ref, input_ref)
    for first in range(0, seq_len, tile):
        span = first + tile
        row, col = col_mask(first, tile, span)
        causal = col <= row
        own = (col // BLOCK) == (row // BLOCK)
        gap = jnp.where(causal, gap_row[:, :span], -jnp.inf)
        top = jnp.max(gap, axis=1, keepdims=True)
        cum = jnp.sum(jnp.where(causal, log_forget[:, :span], 0.0), axis=1, keepdims=True)
        scores = lax.dot_general(
            q_ref[first:span, :],
            k_ref[0:span, :],
            (((1,), (1,)), ((), ())),
            preferred_element_type=jnp.float32,
        ) * width ** (-0.5)
        weights = scores * jnp.exp(gap - top)
        high = weights.astype(jnp.bfloat16)
        high_float = high.astype(jnp.float32)
        low_float = jnp.where(own, 0.0, weights - high_float)
        v = v_ref[0:span, :]
        num_ref[first:span, :] = jnp.dot(high, v, preferred_element_type=jnp.float32) + jnp.dot(
            low_float.astype(jnp.bfloat16), v, preferred_element_type=jnp.float32
        )
        den = jnp.sum(high_float + low_float, axis=1, keepdims=True)
        lane = lax.broadcasted_iota(jnp.int32, (tile, 128), 1)
        aux_ref[first:span, :] = jnp.where(lane == 0, den, jnp.where(lane == 1, top, cum))


def cell_join_kernel(q_ref, num_ref, aux_ref, states_ref, rows_ref, mat_ref, *, axis):
    width = q_ref.shape[1]
    place = lax.axis_index(axis)
    mat_ref[...] = jnp.zeros_like(mat_ref)

    def join(step, carry):
        vector, old_max = carry
        extra = states_ref[step, width : width + EXTRA, :]
        new_max, total = extra[2:3], extra[1:2]
        joined = jnp.maximum(total + old_max, new_max)
        keep_old = jnp.exp(total + old_max - joined)
        keep_new = jnp.exp(new_max - joined)
        mat_ref[...] = keep_old * mat_ref[...] + keep_new * states_ref[step, 0:width, :]
        return keep_old * vector + keep_new * extra[0:1], joined

    vector, far_max = lax.fori_loop(
        0,
        place,
        join,
        (jnp.zeros((1, width), jnp.float32), jnp.full((1, width), FLOOR_LOG, jnp.float32)),
    )
    aux = aux_ref[...]
    den, top, cum = aux[:, 0:1], aux[:, 1:2], aux[:, 2:3]
    far = far_max[:, 0:1]
    joined = jnp.maximum(top, far)
    keep_own = jnp.exp(top - joined)
    keep_far = jnp.exp(far - joined)
    q_float = q_ref[...].astype(jnp.float32)
    one, rest = split_two(mat_ref[...])
    two, three = split_two(mat_ref[...] - one.astype(jnp.float32))
    q = q_ref[...]
    far_num = (
        jnp.dot(q, one, preferred_element_type=jnp.float32)
        + jnp.dot(q, two, preferred_element_type=jnp.float32)
        + jnp.dot(q, three, preferred_element_type=jnp.float32)
    )
    far_den = jnp.sum(q_float * vector, axis=1, keepdims=True)
    numerator = keep_own * num_ref[...] + keep_far * far_num
    denominator = keep_own * den + keep_far * far_den
    divisor = jnp.maximum(jnp.abs(denominator), jnp.exp(-(cum + joined)))
    rows_ref[...] = (numerator / divisor).astype(rows_ref.dtype)


def run_cell(query, keys, values, forget_pre, input_pre):
    seq_len, width = query.shape
    params = pltpu.CompilerParams(vmem_limit_bytes=VMEM_LIMIT)
    state = pl.pallas_call(
        cell_state_kernel,
        out_shape=jax.ShapeDtypeStruct((width + EXTRA, width), jnp.float32),
        compiler_params=params,
        cost_estimate=pl.CostEstimate(flops=10**9, bytes_accessed=2**20, transcendentals=0),
        name="cell_state",
    )(keys, values, forget_pre, input_pre)
    cut = (width + EXTRA) // 3
    parts = [lax.all_gather(state[i * cut : (i + 1) * cut], "sp") for i in range(3)]
    gathered = jnp.concatenate(parts, axis=1)
    tile = 4 * BLOCK if seq_len % (4 * BLOCK) == 0 else BLOCK
    numerator, aux = pl.pallas_call(
        functools.partial(cell_local_kernel, tile=tile),
        out_shape=(
            jax.ShapeDtypeStruct((seq_len, width), jnp.float32),
            jax.ShapeDtypeStruct((seq_len, 128), jnp.float32),
        ),
        compiler_params=params,
        cost_estimate=pl.CostEstimate(flops=5 * 10**9, bytes_accessed=2**21, transcendentals=0),
        name="cell_local",
    )(query, keys, values, forget_pre, input_pre)
    rows = pl.pallas_call(
        functools.partial(cell_join_kernel, axis="sp"),
        out_shape=jax.ShapeDtypeStruct((seq_len, width), jnp.bfloat16),
        scratch_shapes=[pltpu.VMEM((width, width), jnp.float32)],
        compiler_params=params,
        name="cell_join",
    )(query, numerator, aux, gathered)
    return rows


def slot_select(expert_ids, expert_count, capacity):
    flat_ids = expert_ids.reshape(-1)
    one_hot = (flat_ids[:, None] == jnp.arange(expert_count, dtype=jnp.int32)[None, :]).astype(
        jnp.int32
    )
    slot_rank = jnp.sum((jnp.cumsum(one_hot, axis=0) - 1) * one_hot, axis=1)
    target = flat_ids * capacity + slot_rank
    return (
        jnp.arange(expert_count * capacity, dtype=jnp.int32)[:, None] == target[None, :]
    ).astype(jnp.bfloat16)


def exchange_kernel(send_ref, recv_ref, send_sems, recv_sems, own_sem, *, axis, count):
    place = lax.axis_index(axis)
    barrier = pltpu.get_barrier_semaphore()
    for step in range(1, count):
        peer = lax.rem(place + step, count)
        pl.semaphore_signal(
            barrier, inc=1, device_id={axis: peer}, device_id_type=pl.DeviceIdType.MESH
        )
    own = pltpu.make_async_copy(send_ref.at[place], recv_ref.at[place], own_sem)
    own.start()
    pl.semaphore_wait(barrier, count - 1)
    copies = []
    for step in range(1, count):
        peer = lax.rem(place + step, count)
        copy = pltpu.make_async_remote_copy(
            src_ref=send_ref.at[peer],
            dst_ref=recv_ref.at[place],
            send_sem=send_sems.at[step - 1],
            recv_sem=recv_sems.at[step - 1],
            device_id={axis: peer},
            device_id_type=pl.DeviceIdType.MESH,
        )
        copy.start()
        copies.append(copy)
    own.wait()
    for copy in copies:
        copy.wait()


def exchange(blocks, axis, collective_id):
    count = lax.axis_size(axis)
    grouped = blocks.reshape((count, -1) + blocks.shape[2:])
    out = pl.pallas_call(
        functools.partial(exchange_kernel, axis=axis, count=count),
        out_shape=jax.ShapeDtypeStruct(grouped.shape, grouped.dtype),
        in_specs=[pl.BlockSpec(memory_space=pl.ANY)],
        out_specs=pl.BlockSpec(memory_space=pl.ANY),
        scratch_shapes=[
            pltpu.SemaphoreType.DMA((count - 1,)),
            pltpu.SemaphoreType.DMA((count - 1,)),
            pltpu.SemaphoreType.DMA(()),
        ],
        compiler_params=pltpu.CompilerParams(collective_id=collective_id, has_side_effects=True),
        name="exchange",
    )(grouped)
    return out.reshape(blocks.shape)


def run_experts(arrived, w_gate, w_up, w_down, sources):
    local_count = w_gate.shape[0]
    grouped = arrived.reshape(sources, local_count, arrived.shape[1], arrived.shape[2])
    gate_pre = jnp.einsum("pesd,edf->pesf", grouped, w_gate, preferred_element_type=jnp.float32)
    up_pre = jnp.einsum("pesd,edf->pesf", grouped, w_up, preferred_element_type=jnp.float32)
    active = (jax.nn.silu(gate_pre) * up_pre).astype(jnp.bfloat16)
    result = jnp.einsum(
        "pesf,efd->pesd", active, w_down, preferred_element_type=jnp.float32
    ).astype(jnp.bfloat16)
    return result.reshape(arrived.shape)


def shards(
    resid,
    query,
    keys,
    values,
    out_gate,
    forget_pre,
    input_pre,
    head_gain,
    out_proj,
    ffn_gain,
    routes,
    route_scores,
    w_gate,
    w_up,
    w_down,
):
    head_width = query.shape[1]
    row_count, route_count = routes.shape
    sources = lax.axis_size("sp")
    local_experts = w_gate.shape[0]
    expert_count = local_experts * sources
    half_rows = row_count // 2
    capacity = max(2, 2 * half_rows * route_count // expert_count)
    route_weight = route_scores / jnp.sum(route_scores, axis=1, keepdims=True)
    cell_rows = run_cell(query, keys, values, forget_pre, input_pre)
    token_rows = lax.all_to_all(cell_rows, "tp", split_axis=0, concat_axis=1, tiled=True)
    cell_float = token_rows.astype(jnp.float32)
    headed = (
        cell_float
        * lax.rsqrt(jnp.mean(cell_float * cell_float, axis=1, keepdims=True) + EPS)
        * head_gain[None, :]
    )
    gated_out = (headed * jax.nn.sigmoid(out_gate.astype(jnp.float32))).astype(jnp.bfloat16)
    after_mix = resid.astype(jnp.float32) + jnp.dot(
        gated_out, out_proj, preferred_element_type=jnp.float32
    )
    normed_rows = (
        after_mix
        * lax.rsqrt(jnp.mean(after_mix * after_mix, axis=1, keepdims=True) + EPS)
        * ffn_gain[None, :]
    ).astype(jnp.bfloat16)
    selects = [
        slot_select(
            routes[half_idx * half_rows : (half_idx + 1) * half_rows], expert_count, capacity
        )
        for half_idx in range(2)
    ]

    def pack_rows(half_idx):
        selection = (
            selects[half_idx].reshape(expert_count * capacity, half_rows, route_count).sum(axis=2)
        )
        packed = jnp.dot(
            selection,
            normed_rows[half_idx * half_rows : (half_idx + 1) * half_rows],
            preferred_element_type=jnp.float32,
        )
        return packed.astype(jnp.bfloat16).reshape(expert_count, capacity, normed_rows.shape[1])

    send_rows = jnp.concatenate([pack_rows(0), pack_rows(1)], axis=1)
    finished = run_experts(
        exchange(send_rows, "sp", 1),
        w_gate,
        w_up,
        w_down,
        sources,
    )
    returned = exchange(finished, "sp", 2)
    answers = [returned[:, :capacity], returned[:, capacity:]]
    pieces = []
    for half_idx in range(2):
        gathered = lax.dot_general(
            selects[half_idx],
            answers[half_idx].reshape(expert_count * capacity, -1),
            (((0,), (0,)), ((), ())),
            preferred_element_type=jnp.float32,
        )
        weights_half = route_weight[half_idx * half_rows : (half_idx + 1) * half_rows]
        pieces.append(
            jnp.sum(gathered.reshape(half_rows, route_count, -1) * weights_half[:, :, None], axis=1)
        )
    return (after_mix + jnp.concatenate(pieces, axis=0)).astype(jnp.bfloat16)


def solution(mesh):
    placed = (
        P(("sp", "tp"), None),
        P("sp", "tp"),
        P("sp", "tp"),
        P("sp", "tp"),
        P(("sp", "tp"), None),
        P("tp", "sp"),
        P("tp", "sp"),
        P(),
        P(),
        P(),
        P(("sp", "tp"), None),
        P(("sp", "tp"), None),
        P("sp", None, None),
        P("sp", None, None),
        P("sp", None, None),
    )
    return jax.shard_map(
        shards, mesh=mesh, in_specs=placed, out_specs=P(("sp", "tp"), None), check_vma=False
    )
```
